512 devices in a mesh: sp: 32 (over z, x), tp: 16 (over y, core).
Axes of the slice: x: 4, y: 8, z: 8, core: 2. Of those that a mesh axis runs over, the one named last changes fastest.
Arguments:
- cotangent: bfloat16 [4096, 2048], P('sp'), may hold values from -6 to 6
- layer_input: bfloat16 [4096, 2048], P('sp'), may hold values from -6 to 6
- group_choice: int32 [4096], P('sp'), may hold values from 0 to 7, as said below
- inner_pair: int32 [4096, 2], P('sp'), may hold values from 0 to 3, as said below
- group_weight: float32 [4096], P('sp'), may hold values from 0.25 to 1
- inner_logits: float32 [4096, 2], P('sp'), may hold values from -6 to 6
- w_gate: bfloat16 [32, 2048, 2048], P('sp', 'tp'), may hold values from -0.125 to 0.125
- w_up: bfloat16 [32, 2048, 2048], P('sp', 'tp'), may hold values from -0.125 to 0.125
- w_down: bfloat16 [32, 2048, 2048], P('sp', 'tp'), may hold values from -0.125 to 0.125
- outer_gate: bfloat16 [2048, 4096], P('tp', 'sp'), may hold values from -6 to 6
- inner_gate: bfloat16 [2048, 4096], P('tp', 'sp'), may hold values from -6 to 6
- value_stream: bfloat16 [2048, 4096], P('tp', 'sp'), may hold values from -6 to 6
- conv_out: bfloat16 [2048, 4096], P('tp', 'sp'), may hold values from -6 to 6
- conv_taps: float32 [3, 2048], P(None, 'tp'), may hold values from -4 to 4
- w_out: bfloat16 [2048, 2048], P(None, 'tp'), may hold values from -0.125 to 0.125
Outputs:
- grad_input: bfloat16 [4096, 2048], P('sp', 'tp')
- grad_w_gate: bfloat16 [32, 2048, 2048], P('sp', 'tp')
- grad_w_up: bfloat16 [32, 2048, 2048], P('sp', 'tp')
- grad_w_down: bfloat16 [32, 2048, 2048], P('sp', 'tp')
- grad_w_out: float32 [2048, 2048], P('sp', 'tp')
- grad_outer_gate: bfloat16 [2048, 4096], P('tp', 'sp')
- grad_inner_gate: bfloat16 [2048, 4096], P('tp', 'sp')
- grad_value_stream: bfloat16 [2048, 4096], P('tp', 'sp')
The draws below stay inside these ranges and needn't reach their ends.
Inputs may be any that keep to these rules, and one draw needn't show every extreme that they name: Within each block of 128 positions of the sp order, every expert 4 * group_choice + inner_pair is named by at most 16 positions; in every block the 4 experts of one group, the same group for all blocks, are each named by exactly 16 positions. `inner_pair`: the two entries of a position differ.
All inputs are finite; a program needn't handle non-finite values.
Results may differ from the reference program's by a relative error of at most 0.019.
Values may be sent and summed in bfloat16 or wider, within the bound.
No kernel may reach another device: no remote copies, remote signals or barrier semaphores. Data moves between devices by JAX's collectives and lax.ppermute only.
A program may use at most 64 MiB of HBM per device.

```python
import math
import jax
import jax.numpy as jnp
from jax import lax

D = 2048
FF = 2048
W = 2048
TAPS = 3
INNER = 4
TOK_DEV = 128
TOKENS = 4096
EXPERTS = 32
GROUPS = 8
CAP = 16
HID_BLOCKS = 16


def route_plan(key):
    blocks = TOKENS // TOK_DEV
    group_span = 2 * CAP
    slot_count = GROUPS * group_span
    full_group = jax.random.randint(jax.random.fold_in(key, 7001), (), 0, GROUPS)

    def one_block(block):
        block_key = jax.random.fold_in(key, block)
        ranking = jax.random.permutation(jax.random.fold_in(block_key, 1), slot_count).astype(jnp.int32)
        owning = jnp.arange(slot_count, dtype=jnp.int32) // group_span
        scores = jnp.where(owning == full_group, ranking - slot_count, ranking)
        chosen = jnp.argsort(scores, stable=True)[:TOK_DEV].astype(jnp.int32)
        shuffle = jax.random.permutation(jax.random.fold_in(block_key, 2), TOK_DEV)
        chosen = chosen[shuffle]
        group_ids = chosen // group_span
        within = chosen % group_span
        first_pick = within % 4
        second_pick = (first_pick + 1 + within // 4 % 3) % 4
        rotation = jax.random.randint(jax.random.fold_in(block_key, 3), (GROUPS,), 0, 4)[group_ids]
        picks = jnp.stack([(first_pick + rotation) % 4, (second_pick + rotation) % 4], axis=1)
        return (group_ids.astype(jnp.int32), picks.astype(jnp.int32))
    group_ids, picks = jax.vmap(one_block)(jnp.arange(blocks))
    return (group_ids.reshape(TOKENS), picks.reshape(TOKENS, 2))


def draw_group_choice(key, part):
    return route_plan(key)[0]


def draw_inner_pair(key, part):
    return route_plan(key)[1]


def spiked(values, stream_key, source, target, blocks, factor):
    def block_of(axis_at):
        return (jnp.arange(values.shape[axis_at]) // (values.shape[axis_at] // blocks)).reshape((-1,) + (1,) * (values.ndim - 1 - axis_at))

    near = jax.random.permutation(stream_key, blocks)[block_of(target)]
    other_side = (block_of(target) + blocks // 2) % blocks
    return jnp.where((block_of(source) == near) | (block_of(source) == other_side), factor * values, values)


def block_scale(stream_key, shape, cuts, least, high):
    def one(dim, shards_of):
        draws = jax.random.uniform(jax.random.fold_in(jax.random.fold_in(stream_key, 6), dim), (shards_of,), jnp.float32, least / len(cuts), high / len(cuts))
        return jnp.repeat(jnp.exp(draws), shape[dim] // shards_of).reshape((-1,) + (1,) * (len(shape) - dim - 1))

    loudness = one(*cuts[0])
    for cut in cuts[1:]:
        loudness = loudness * one(*cut)
    return loudness


def centred(own_key, extent, deviation, bound, split=(), kind=jnp.bfloat16):
    array = jax.random.normal(own_key, extent, jnp.float32) * deviation
    if len(split) > 0:
        array = block_scale(own_key, extent, split, -0.22, 0.18) * array
    return jnp.clip(array, min=-bound, max=bound).astype(kind)


def noise_with(rng, dims, deviation, bound, shards, heavy, kind=jnp.bfloat16):
    values = deviation * jax.random.normal(rng, dims, jnp.float32)
    if shards:
        values = values * block_scale(rng, dims, shards, -0.22, 0.18)
    return jnp.clip(spiked(values, jax.random.fold_in(rng, 3), *heavy), -bound, bound).astype(kind)


def setup_inputs(seed: int = 0) -> dict:
    arg_keys = jax.random.split(jax.random.key(seed), 16)
    cotangent = noise_with(arg_keys[0], (TOKENS, D), 1.0, 6.0, ((0, 32),), (0, 1, 32, 2.75))
    layer_input = centred(arg_keys[1], (TOKENS, D), 1.0, 6.0, ((0, 32),))
    group_choice = draw_group_choice(jax.random.fold_in(arg_keys[15], 71), 0)
    inner_pair = draw_inner_pair(jax.random.fold_in(arg_keys[15], 71), 0)
    group_weight = jnp.clip(jnp.exp(math.log(1.0) - 1.3862944 * jax.random.uniform(arg_keys[4], (TOKENS,), jnp.float32) ** block_scale(arg_keys[4], (TOKENS,), ((0, 32),), -0.2, 0.2)), 0.25, 1.0)
    inner_logits = centred(arg_keys[5], (TOKENS, 2), 1.5, 6.0, ((0, 32),), jnp.float32)
    w_gate = centred(arg_keys[6], (EXPERTS, FF, D), D ** -0.5, 0.125, ((0, 32), (1, 16)))
    w_up = centred(arg_keys[7], (EXPERTS, FF, D), D ** -0.5, 0.125, ((0, 32), (1, 16)))
    w_down = centred(arg_keys[8], (EXPERTS, FF, D), FF ** -0.5, 0.125, ((0, 32), (1, 16)))
    outer_gate = centred(arg_keys[9], (W, TOKENS), 1.0, 6.0, ((0, 16), (1, 32)))
    inner_gate = centred(arg_keys[10], (W, TOKENS), 1.0, 6.0, ((0, 16), (1, 32)))
    value_stream = centred(arg_keys[11], (W, TOKENS), 1.0, 6.0, ((0, 16), (1, 32)))
    conv_out = centred(arg_keys[12], (W, TOKENS), 1.0, 6.0, ((0, 16), (1, 32)))
    conv_taps = centred(arg_keys[13], (TAPS, W), 0.6, 4.0, ((1, 16),), jnp.float32)
    w_out = centred(arg_keys[14], (D, W), W ** -0.5, 0.125, ((1, 16),))
    return {"cotangent": cotangent, "layer_input": layer_input, "group_choice": group_choice, "inner_pair": inner_pair, "group_weight": group_weight, "inner_logits": inner_logits, "w_gate": w_gate, "w_up": w_up, "w_down": w_down, "outer_gate": outer_gate, "inner_gate": inner_gate, "value_stream": value_stream, "conv_out": conv_out, "conv_taps": conv_taps, "w_out": w_out}


def slot_table(group_choice, inner_pair):
    expert_ids = (INNER * group_choice[:, None] + inner_pair).astype(jnp.int32)
    blocks = TOKENS // TOK_DEV
    flat_ids = expert_ids.reshape(blocks, TOK_DEV * 2)
    onehot = (flat_ids[:, :, None] == jnp.arange(EXPERTS, dtype=jnp.int32)[None, None, :]).astype(jnp.int32)
    position = jnp.sum((jnp.cumsum(onehot, axis=1) - onehot) * onehot, axis=2).astype(jnp.int32)
    entries = jnp.arange(TOKENS * 2, dtype=jnp.int32).reshape(blocks, TOK_DEV * 2)
    source = jnp.broadcast_to(jnp.arange(blocks, dtype=jnp.int32)[:, None], flat_ids.shape)
    slot_map = jnp.full((EXPERTS, blocks, CAP), -1, jnp.int32)
    slot_map = slot_map.at[flat_ids, source, position].set(entries)
    return slot_map.reshape(EXPERTS, blocks * CAP)


def reference(cotangent, layer_input, group_choice, inner_pair, group_weight, inner_logits,
              w_gate, w_up, w_down, outer_gate, inner_gate, value_stream, conv_out, conv_taps, w_out):
    slot_map = slot_table(group_choice, inner_pair)
    route = group_weight[:, None] * jax.nn.softmax(inner_logits, axis=1)
    scaled = (route[:, :, None] * cotangent.astype(jnp.float32)[:, None, :]).astype(jnp.bfloat16)
    scaled = scaled.reshape(TOKENS * 2, D)
    rows_in = jnp.repeat(layer_input, 2, axis=0)
    inner_dims = (((1,), (1,)), ((), ()))
    row_dims = (((0,), (0,)), ((), ()))
    block_width = FF // HID_BLOCKS

    def expert_pass(inputs):
        slot_index, gate_weight, up_weight, down_weight = inputs
        filled = slot_index >= 0
        clamped = jnp.maximum(slot_index, 0)
        in_rows = jnp.where(filled[:, None], rows_in[clamped], jnp.zeros((), jnp.bfloat16))
        scaled_rows = jnp.where(filled[:, None], scaled[clamped], jnp.zeros((), jnp.bfloat16))
        gate_pre = lax.dot_general(in_rows, gate_weight, inner_dims, preferred_element_type=jnp.float32)
        up_pre = lax.dot_general(in_rows, up_weight, inner_dims, preferred_element_type=jnp.float32)
        back = lax.dot_general(scaled_rows, down_weight, inner_dims, preferred_element_type=jnp.float32)
        sigmoid_gate = jax.nn.sigmoid(gate_pre)
        silu_gate = gate_pre * sigmoid_gate
        hidden = (silu_gate * up_pre).astype(jnp.bfloat16)
        grad_gate = (back * up_pre * sigmoid_gate * (1.0 + gate_pre * (1.0 - sigmoid_gate))).astype(jnp.bfloat16)
        grad_up = (back * silu_gate).astype(jnp.bfloat16)
        gate_grad = lax.dot_general(grad_gate, in_rows, row_dims, preferred_element_type=jnp.float32).astype(jnp.bfloat16)
        up_grad = lax.dot_general(grad_up, in_rows, row_dims, preferred_element_type=jnp.float32).astype(jnp.bfloat16)
        down_grad = lax.dot_general(hidden, scaled_rows, row_dims, preferred_element_type=jnp.float32).astype(jnp.bfloat16)
        blocked_gate = grad_gate.astype(jnp.float32).reshape(-1, HID_BLOCKS, block_width)
        blocked_up = grad_up.astype(jnp.float32).reshape(-1, HID_BLOCKS, block_width)
        gate_blocks = gate_weight.astype(jnp.float32).reshape(HID_BLOCKS, block_width, D)
        up_blocks = up_weight.astype(jnp.float32).reshape(HID_BLOCKS, block_width, D)
        pieces = jnp.einsum("rbf,bfd->rbd", blocked_gate, gate_blocks) + jnp.einsum("rbf,bfd->rbd", blocked_up, up_blocks)
        pieces = lax.optimization_barrier(pieces.astype(jnp.bfloat16)).astype(jnp.float32)
        returned = jnp.sum(pieces, axis=1).astype(jnp.bfloat16)
        return gate_grad, up_grad, down_grad, returned

    grad_w_gate, grad_w_up, grad_w_down, returned = lax.map(expert_pass, (slot_map, w_gate, w_up, w_down))
    targets = jnp.where(slot_map >= 0, slot_map, 2 * TOKENS).reshape(-1).astype(jnp.int32)
    collected = jnp.zeros((2 * TOKENS, D), jnp.float32).at[targets].set(
        returned.reshape(-1, D).astype(jnp.float32), mode="drop")
    collected = collected.reshape(TOKENS, 2, D)
    grad_input = (cotangent.astype(jnp.float32) + collected[:, 0] + collected[:, 1]).astype(jnp.bfloat16)

    grad_out = lax.dot_general(w_out, grad_input, (((0,), (1,)), ((), ())), preferred_element_type=jnp.float32)
    mixer_out = (outer_gate.astype(jnp.float32) * conv_out.astype(jnp.float32)).astype(jnp.bfloat16)
    grad_w_out = lax.dot_general(grad_input, mixer_out, (((0,), (1,)), ((), ())), preferred_element_type=jnp.float32)
    grad_outer_gate = (grad_out * conv_out.astype(jnp.float32)).astype(jnp.bfloat16)
    grad_conv = grad_out * outer_gate.astype(jnp.float32)
    extended = jnp.pad(grad_conv, ((0, 0), (0, TAPS - 1)))
    grad_mixed = jnp.zeros_like(grad_conv)
    for offset in range(TAPS):
        start = TAPS - 1 - offset
        grad_mixed = grad_mixed + conv_taps[offset][:, None] * extended[:, start:start + TOKENS]
    grad_inner_gate = (grad_mixed * value_stream.astype(jnp.float32)).astype(jnp.bfloat16)
    grad_value_stream = (grad_mixed * inner_gate.astype(jnp.float32)).astype(jnp.bfloat16)
    return (grad_input, grad_w_gate, grad_w_up, grad_w_down, grad_w_out,
            grad_outer_gate, grad_inner_gate, grad_value_stream)
```

```python
import jax
import jax.numpy as jnp
from jax import lax
from jax.experimental import pallas as pl
from jax.experimental.pallas import tpu as pltpu
from jax.sharding import PartitionSpec as P

TAPS = 3
INNER = 4
BF = jnp.bfloat16
F32 = jnp.float32


def dot(a, b, ca, cb):
    return lax.dot_general(a, b, (((ca,), (cb,)), ((), ())), preferred_element_type=F32)


def pack_kernel(place, group, pair, weight, logits, rows, cots, rows_out, scaled_out, slots_out):
    half, core = place[0], place[1]
    tokens, width = rows.shape[0], rows_out.shape[1]
    slots = rows_out.shape[0]
    experts = slots // 8
    first = INNER * group[...] + pair[0:1, :]
    second = INNER * group[...] + pair[1:2, :]
    kind = lax.broadcasted_iota(jnp.int32, (experts, tokens), 0)
    named_first = (kind == first).astype(F32)
    named_second = (kind == second).astype(F32)
    before = (
        lax.broadcasted_iota(jnp.int32, (tokens, tokens), 0)
        < lax.broadcasted_iota(jnp.int32, (tokens, tokens), 1)
    ).astype(BF)
    rank = dot((named_first + named_second).astype(BF), before, 1, 0)
    rank_first = jnp.sum(rank * named_first, axis=0, keepdims=True).astype(jnp.int32) - 8 * core
    rank_second = jnp.sum(rank * named_second, axis=0, keepdims=True).astype(jnp.int32) - 8 * core
    at_first = jnp.where((rank_first >= 0) & (rank_first < 8), first * 8 + rank_first, -1)
    at_second = jnp.where((rank_second >= 0) & (rank_second < 8), second * 8 + rank_second, -1)
    top = jnp.maximum(logits[0:1, :], logits[1:2, :])
    exp_first = jnp.exp(logits[0:1, :] - top)
    exp_second = jnp.exp(logits[1:2, :] - top)
    share = weight[...] / (exp_first + exp_second)
    slot = lax.broadcasted_iota(jnp.int32, (slots, tokens), 0)
    is_first, is_second = slot == at_first, slot == at_second
    routing = jnp.sum(
        jnp.where(is_first, share * exp_first, jnp.where(is_second, share * exp_second, 0.0)),
        axis=1,
        keepdims=True,
    )
    pick = jnp.where(is_first | is_second, 1.0, 0.0).astype(BF)
    slots_out[...] = pick
    cols = pl.ds(pl.multiple_of(half * width, width), width)
    rows_out[...] = dot(pick, rows[:, cols], 1, 0).astype(BF)
    scaled_out[...] = (dot(pick, cots[:, cols], 1, 0) * routing).astype(BF)


def expert_kernel(place, own_in, far_in, own_sc, far_sc, weights, part, grad_g, grad_u, hid):
    half = place[0]
    width = own_in.shape[1]
    own = pl.ds(pl.multiple_of(half * width, width), width)
    far = pl.ds(pl.multiple_of((1 - half) * width, width), width)

    def full(a, b, k):
        return dot(a[...], weights[k, :, own], 1, 1) + dot(b[...], weights[k, :, far], 1, 1)

    gate_pre, up_pre, back = full(own_in, far_in, 0), full(own_in, far_in, 1), full(own_sc, far_sc, 2)
    sig = jax.nn.sigmoid(gate_pre)
    silu = gate_pre * sig
    hid[...] = (silu * up_pre).astype(BF)
    gg = (back * up_pre * sig * (1.0 + gate_pre * (1.0 - sig))).astype(BF)
    gu = (back * silu).astype(BF)
    grad_g[...] = gg
    grad_u[...] = gu
    block = part.shape[2]
    for j in range(part.shape[0]):
        cols = slice(j * block, (j + 1) * block)
        part[j] = (dot(gg, weights[0, :, cols], 1, 0) + dot(gu, weights[1, :, cols], 1, 0)).astype(BF)


def weight_grad_kernel(place, grad_g, grad_u, hid, own_in, far_in, own_sc, far_sc, keep, send):
    half = place[0]
    width = own_in.shape[1]
    rows = keep.shape[1]
    own = pl.ds(pl.multiple_of(half * width, width), width)
    far = pl.ds(pl.multiple_of((1 - half) * width, width), width)
    for k, (left, a, b) in enumerate(
        ((grad_g, own_in, far_in), (grad_u, own_in, far_in), (hid, own_sc, far_sc))
    ):
        for right, cols in ((a, own), (b, far)):
            both = dot(left[...], right[...], 0, 0)
            keep[k, :, cols] = both[:rows]
            send[k, :, cols] = both[rows:].astype(BF)


def call(kernel, outs, *args):
    vmem = pl.BlockSpec(memory_space=pltpu.VMEM)
    return pl.pallas_call(
        kernel,
        out_shape=tuple(jax.ShapeDtypeStruct(s, d) for s, d in outs),
        in_specs=[pl.BlockSpec(memory_space=pltpu.SMEM)] + [vmem] * (len(args) - 1),
        out_specs=tuple(vmem for _ in outs),
    )(*args)


def per_device(
    cotangent,
    layer_input,
    group_choice,
    inner_pair,
    group_weight,
    inner_logits,
    w_gate,
    w_up,
    w_down,
    outer_gate,
    inner_gate,
    value_stream,
    conv_out,
    conv_taps,
    w_out,
):
    sp, tp = lax.axis_size("sp"), lax.axis_size("tp")
    at = lax.axis_index("tp")
    chip, core = at // 2, at % 2
    tok, width = cotangent.shape
    hidden = w_gate.shape[1]
    half_width = width // 2
    slots = sp * 8
    col = width // tp
    place = jnp.stack([chip % 2, core]).astype(jnp.int32)
    swap = [(i, i ^ 1) for i in range(tp)]
    onward = [(i, (i + 2 - 4 * (i % 2)) % tp) for i in range(tp)]
    lines = [list(range(c, tp, 2)) for c in range(2)]

    in_send, sc_send, pick = call(
        pack_kernel,
        [((slots, half_width), BF), ((slots, half_width), BF), ((slots, tok), BF)],
        place,
        group_choice[None, :],
        inner_pair.T,
        group_weight[None, :],
        inner_logits.T,
        layer_input,
        cotangent,
    )

    def dispatched(x):
        y = lax.all_to_all(x.reshape(sp, 8, half_width), "sp", 0, 0, tiled=True)
        return y.reshape(slots, half_width)

    own_in, own_sc = dispatched(in_send), dispatched(sc_send)
    mine = jnp.concatenate([w_gate, w_up, w_down], axis=0)
    theirs = lax.ppermute(mine, "tp", swap)
    weights = jnp.concatenate([mine, theirs], axis=1)
    far_in = lax.ppermute(own_in, "tp", onward)
    far_sc = lax.ppermute(own_sc, "tp", onward)
    part, grad_g, grad_u, hid = call(
        expert_kernel,
        [((tp // 2, slots, 2 * col), BF)] + [((slots, 2 * hidden), BF)] * 3,
        place,
        own_in,
        far_in,
        own_sc,
        far_sc,
        weights,
    )
    parts = lax.all_to_all(part, "tp", 0, 0, axis_index_groups=lines, tiled=True)
    keep, send = call(
        weight_grad_kernel,
        [((3, hidden, width), F32), ((3, hidden, width), BF)],
        place,
        grad_g,
        grad_u,
        hid,
        own_in,
        far_in,
        own_sc,
        far_sc,
    )
    grad_w = (keep + lax.ppermute(send, "tp", swap).astype(F32)).astype(BF)
    shares = jnp.sum(parts.astype(F32), axis=0).astype(BF)
    returned = lax.all_to_all(shares.reshape(sp, 8, 2 * col), "sp", 0, 0, tiled=True)
    back = dot(pick, returned.reshape(slots, 2 * col), 0, 0)
    back_mine = jnp.where(core == 0, back[:, :col], back[:, col:])
    back_theirs = jnp.where(core == 0, back[:, col:], back[:, :col])
    back_other = lax.ppermute(back_theirs, "tp", swap)
    cot_cols = lax.dynamic_slice_in_dim(cotangent, at * col, col, 1).astype(F32)
    own_cols = (cot_cols + back_mine + back_other).astype(BF)
    grad_rows = lax.all_gather(own_cols, "tp", axis=1, tiled=True)
    mixer_out = (outer_gate.astype(F32) * conv_out.astype(F32)).astype(BF)
    partial_out = dot(grad_rows, mixer_out, 0, 1).astype(BF)
    blocks = lax.all_to_all(partial_out.reshape(sp, width // sp, -1), "sp", 0, 0, tiled=True)
    grad_w_out = jnp.sum(blocks.astype(F32), axis=0)
    grad_out = dot(w_out, grad_rows, 0, 1)
    grad_outer_gate = (grad_out * conv_out.astype(F32)).astype(BF)
    grad_conv = grad_out * outer_gate.astype(F32)
    following = lax.ppermute(grad_conv[:, : TAPS - 1], "sp", [(i + 1, i) for i in range(sp - 1)])
    extended = jnp.concatenate([grad_conv, following], axis=1)
    grad_mixed = jnp.zeros_like(grad_conv)
    for offset in range(TAPS):
        start = TAPS - 1 - offset
        grad_mixed = grad_mixed + conv_taps[offset][:, None] * extended[:, start : start + tok]
    grad_inner_gate = (grad_mixed * value_stream.astype(F32)).astype(BF)
    grad_value_stream = (grad_mixed * inner_gate.astype(F32)).astype(BF)
    return (
        own_cols,
        grad_w[0:1],
        grad_w[1:2],
        grad_w[2:3],
        grad_w_out,
        grad_outer_gate,
        grad_inner_gate,
        grad_value_stream,
    )


def solution(mesh):
    tokens, experts, channels = P("sp", None), P("sp", "tp", None), P("tp", "sp")
    return jax.shard_map(
        per_device,
        mesh=mesh,
        in_specs=(tokens, tokens, P("sp"), tokens, P("sp"), tokens)
        + (experts,) * 3
        + (channels,) * 4
        + (P(None, "tp"), P(None, "tp")),
        out_specs=(P("sp", "tp"),) + (experts,) * 3 + (P("sp", "tp"),) + (channels,) * 3,
        check_vma=False,
    )
```

```python
import jax
import jax.numpy as jnp
from jax import lax
from jax.experimental import pallas as pl
from jax.experimental.pallas import tpu as pltpu
from jax.sharding import PartitionSpec as P

TAPS = 3
INNER = 4
BLOCK = 256
BF = jnp.bfloat16
F32 = jnp.float32


def dot(a, b, ca, cb):
    return lax.dot_general(a, b, (((ca,), (cb,)), ((), ())), preferred_element_type=F32)


def pack_kernel(place, group, pair, weight, logits, rows, cots, rows_out, scaled_out, slots_out):
    half, core = place[0], place[1]
    tokens, width = rows.shape[0], rows_out.shape[1]
    slots = rows_out.shape[0]
    experts = slots // 8
    first = INNER * group[...] + pair[0:1, :]
    second = INNER * group[...] + pair[1:2, :]
    kind = lax.broadcasted_iota(jnp.int32, (experts, tokens), 0)
    named_first = (kind == first).astype(F32)
    named_second = (kind == second).astype(F32)
    before = (
        lax.broadcasted_iota(jnp.int32, (tokens, tokens), 0)
        < lax.broadcasted_iota(jnp.int32, (tokens, tokens), 1)
    ).astype(BF)
    rank = dot((named_first + named_second).astype(BF), before, 1, 0)
    rank_first = jnp.sum(rank * named_first, axis=0, keepdims=True).astype(jnp.int32) - 8 * core
    rank_second = jnp.sum(rank * named_second, axis=0, keepdims=True).astype(jnp.int32) - 8 * core
    at_first = jnp.where((rank_first >= 0) & (rank_first < 8), first * 8 + rank_first, -1)
    at_second = jnp.where((rank_second >= 0) & (rank_second < 8), second * 8 + rank_second, -1)
    top = jnp.maximum(logits[0:1, :], logits[1:2, :])
    exp_first = jnp.exp(logits[0:1, :] - top)
    exp_second = jnp.exp(logits[1:2, :] - top)
    share = weight[...] / (exp_first + exp_second)
    slot = lax.broadcasted_iota(jnp.int32, (slots, tokens), 0)
    is_first, is_second = slot == at_first, slot == at_second
    routing = jnp.sum(
        jnp.where(is_first, share * exp_first, jnp.where(is_second, share * exp_second, 0.0)),
        axis=1,
        keepdims=True,
    )
    pick = jnp.where(is_first | is_second, 1.0, 0.0).astype(BF)
    slots_out[...] = pick
    for here, there in pieces(width, half):
        rows_out[:, here] = dot(pick, rows[:, there], 1, 0).astype(BF)
        scaled_out[:, here] = (dot(pick, cots[:, there], 1, 0) * routing).astype(BF)


def pieces(width, half):
    for k in range(width // BLOCK):
        start = pl.multiple_of((2 * k + half) * BLOCK, BLOCK)
        yield slice(k * BLOCK, (k + 1) * BLOCK), pl.ds(start, BLOCK)


def both_halves(own, far, weights, k, half):
    total = 0.0
    for part, side in ((own, half), (far, 1 - half)):
        for here, there in pieces(part.shape[1], side):
            total = total + dot(part[:, here], weights[k, :, there], 1, 1)
    return total


def gate_kernel(place, own_in, far_in, weights, gate_factor, silu_out, hid):
    gate_pre = both_halves(own_in, far_in, weights, 0, place[0])
    up_pre = both_halves(own_in, far_in, weights, 1, place[0])
    sig = jax.nn.sigmoid(gate_pre)
    silu = gate_pre * sig
    hid[...] = (silu * up_pre).astype(BF)
    silu_out[...] = silu
    gate_factor[...] = up_pre * sig * (1.0 + gate_pre * (1.0 - sig))


def back_kernel(place, own_sc, far_sc, weights, gate_factor, silu, far_part, grad_g, grad_u):
    back = both_halves(own_sc, far_sc, weights, 2, place[0])
    gg = (back * gate_factor[...]).astype(BF)
    gu = (back * silu[...]).astype(BF)
    grad_g[...] = gg
    grad_u[...] = gu
    for here, there in pieces(far_part.shape[1], 1 - place[0]):
        far_part[:, here] = (
            dot(gg, weights[0, :, there], 1, 0) + dot(gu, weights[1, :, there], 1, 0)
        ).astype(BF)


def own_part_kernel(place, grad_g, grad_u, weights, own_part):
    for here, there in pieces(own_part.shape[1], place[0]):
        own_part[:, here] = dot(grad_g[...], weights[0, :, there], 1, 0) + dot(
            grad_u[...], weights[1, :, there], 1, 0
        )


def combine_kernel(place, pick, returned, blocks):
    col = blocks.shape[2]
    both = dot(pick[...], returned[...], 0, 0)
    for j in range(blocks.shape[0]):
        blocks[j] = both[:, j * col : (j + 1) * col].astype(BF)


def weight_grad_kernel(place, grad_g, grad_u, hid, own_in, far_in, own_sc, far_sc, keep, send):
    rows = keep.shape[1]
    for k, (left, own, far) in enumerate(
        ((grad_g, own_in, far_in), (grad_u, own_in, far_in), (hid, own_sc, far_sc))
    ):
        for right, side in ((own, place[0]), (far, 1 - place[0])):
            both = dot(left[...], right[...], 0, 0)
            for here, there in pieces(right.shape[1], side):
                keep[k, :, there] = both[:rows, here]
                send[k, :, there] = both[rows:, here].astype(BF)


def call(kernel, outs, *args):
    vmem = pl.BlockSpec(memory_space=pltpu.VMEM)
    return pl.pallas_call(
        kernel,
        out_shape=tuple(jax.ShapeDtypeStruct(s, d) for s, d in outs),
        in_specs=[pl.BlockSpec(memory_space=pltpu.SMEM)] + [vmem] * (len(args) - 1),
        out_specs=tuple(vmem for _ in outs),
    )(*args)


def per_device(
    cotangent,
    layer_input,
    group_choice,
    inner_pair,
    group_weight,
    inner_logits,
    w_gate,
    w_up,
    w_down,
    outer_gate,
    inner_gate,
    value_stream,
    conv_out,
    conv_taps,
    w_out,
):
    sp, tp = lax.axis_size("sp"), lax.axis_size("tp")
    at = lax.axis_index("tp")
    chip, core = at // 2, at % 2
    tok, width = cotangent.shape
    hidden = w_gate.shape[1]
    half_width = width // 2
    slots = sp * 8
    col = width // tp
    place = jnp.stack([chip % 2, core]).astype(jnp.int32)
    swap = [(i, i ^ 1) for i in range(tp)]
    onward = [(i, (i + 2 - 4 * (i % 2)) % tp) for i in range(tp)]
    alike = [[t for t in range(tp) if t // 2 % 2 == p] for p in range(2)]

    in_send, sc_send, pick = call(
        pack_kernel,
        [((slots, half_width), BF), ((slots, half_width), BF), ((slots, tok), BF)],
        place,
        group_choice[None, :],
        inner_pair.T,
        group_weight[None, :],
        inner_logits.T,
        layer_input,
        cotangent,
    )

    def dispatched(x):
        y = lax.all_to_all(x.reshape(sp, 8, half_width), "sp", 0, 0, tiled=True)
        return y.reshape(slots, half_width)

    own_in, own_sc = dispatched(in_send), dispatched(sc_send)
    mine = jnp.concatenate([w_gate, w_up, w_down], axis=0)
    theirs = lax.ppermute(mine, "tp", swap)
    weights = jnp.concatenate([mine, theirs], axis=1)
    far_in = lax.ppermute(own_in, "tp", onward)
    far_sc = lax.ppermute(own_sc, "tp", onward)
    gate_factor, silu, hid = call(
        gate_kernel,
        [((slots, 2 * hidden), F32), ((slots, 2 * hidden), F32), ((slots, 2 * hidden), BF)],
        place,
        own_in,
        far_in,
        weights,
    )
    far_part, grad_g, grad_u = call(
        back_kernel,
        [((slots, half_width), BF)] + [((slots, 2 * hidden), BF)] * 2,
        place,
        own_sc,
        far_sc,
        weights,
        gate_factor,
        silu,
    )
    near_part = lax.ppermute(far_part, "tp", onward)
    (own_part,) = call(
        own_part_kernel, [((slots, half_width), F32)], place, grad_g, grad_u, weights
    )
    halves = (own_part + near_part.astype(F32)).astype(BF)
    returned = lax.all_to_all(halves.reshape(sp, 8, half_width), "sp", 0, 0, tiled=True)
    keep, send = call(
        weight_grad_kernel,
        [((3, hidden, width), F32), ((3, hidden, width), BF)],
        place,
        grad_g,
        grad_u,
        hid,
        own_in,
        far_in,
        own_sc,
        far_sc,
    )
    grad_w = (keep + lax.ppermute(send, "tp", swap).astype(F32)).astype(BF)
    (blocks,) = call(
        combine_kernel,
        [((tp // 2, tok, col), BF)],
        place,
        pick,
        returned.reshape(slots, half_width),
    )
    parts = lax.all_to_all(blocks, "tp", 0, 0, axis_index_groups=alike, tiled=True)
    cot_cols = lax.dynamic_slice_in_dim(cotangent, at * col, col, 1).astype(F32)
    own_cols = (cot_cols + jnp.sum(parts.astype(F32), axis=0)).astype(BF)
    grad_rows = lax.all_gather(own_cols, "tp", axis=1, tiled=True)
    mixer_out = (outer_gate.astype(F32) * conv_out.astype(F32)).astype(BF)
    partial_out = dot(grad_rows, mixer_out, 0, 1).astype(BF)
    sums = lax.all_to_all(partial_out.reshape(sp, width // sp, -1), "sp", 0, 0, tiled=True)
    grad_w_out = jnp.sum(sums.astype(F32), axis=0)
    grad_out = dot(w_out, grad_rows, 0, 1)
    grad_outer_gate = (grad_out * conv_out.astype(F32)).astype(BF)
    grad_conv = grad_out * outer_gate.astype(F32)
    following = lax.ppermute(grad_conv[:, : TAPS - 1], "sp", [(i + 1, i) for i in range(sp - 1)])
    extended = jnp.concatenate([grad_conv, following], axis=1)
    grad_mixed = jnp.zeros_like(grad_conv)
    for offset in range(TAPS):
        start = TAPS - 1 - offset
        grad_mixed = grad_mixed + conv_taps[offset][:, None] * extended[:, start : start + tok]
    grad_inner_gate = (grad_mixed * value_stream.astype(F32)).astype(BF)
    grad_value_stream = (grad_mixed * inner_gate.astype(F32)).astype(BF)
    return (
        own_cols,
        grad_w[0:1],
        grad_w[1:2],
        grad_w[2:3],
        grad_w_out,
        grad_outer_gate,
        grad_inner_gate,
        grad_value_stream,
    )


def solution(mesh):
    tokens, experts, channels = P("sp", None), P("sp", "tp", None), P("tp", "sp")
    return jax.shard_map(
        per_device,
        mesh=mesh,
        in_specs=(tokens, tokens, P("sp"), tokens, P("sp"), tokens)
        + (experts,) * 3
        + (channels,) * 4
        + (P(None, "tp"), P(None, "tp")),
        out_specs=(P("sp", "tp"),) + (experts,) * 3 + (P("sp", "tp"),) + (channels,) * 3,
        check_vma=False,
    )
```

```python
import jax
import jax.numpy as jnp
from jax import lax
from jax.experimental import pallas as pl
from jax.experimental.pallas import tpu as pltpu
from jax.sharding import PartitionSpec as P

TAPS = 3
INNER = 4
BF = jnp.bfloat16
F32 = jnp.float32


def dot(a, b, ca, cb):
    return lax.dot_general(a, b, (((ca,), (cb,)), ((), ())), preferred_element_type=F32)


def pack_kernel(place, group, pair, weight, logits, rows, cots, packed, slots_out):
    half, core = place[0], place[1]
    tokens, width = rows.shape[0], packed.shape[1] // 2
    slots = packed.shape[0]
    experts = slots // 8
    first = INNER * group[...] + pair[0:1, :]
    second = INNER * group[...] + pair[1:2, :]
    kind = lax.broadcasted_iota(jnp.int32, (experts, tokens), 0)
    named_first = (kind == first).astype(F32)
    named_second = (kind == second).astype(F32)
    before = (
        lax.broadcasted_iota(jnp.int32, (tokens, tokens), 0)
        < lax.broadcasted_iota(jnp.int32, (tokens, tokens), 1)
    ).astype(BF)
    rank = dot((named_first + named_second).astype(BF), before, 1, 0)
    rank_first = jnp.sum(rank * named_first, axis=0, keepdims=True).astype(jnp.int32) - 8 * core
    rank_second = jnp.sum(rank * named_second, axis=0, keepdims=True).astype(jnp.int32) - 8 * core
    at_first = jnp.where((rank_first >= 0) & (rank_first < 8), first * 8 + rank_first, -1)
    at_second = jnp.where((rank_second >= 0) & (rank_second < 8), second * 8 + rank_second, -1)
    top = jnp.maximum(logits[0:1, :], logits[1:2, :])
    exp_first = jnp.exp(logits[0:1, :] - top)
    exp_second = jnp.exp(logits[1:2, :] - top)
    share = weight[...] / (exp_first + exp_second)
    slot = lax.broadcasted_iota(jnp.int32, (slots, tokens), 0)
    is_first, is_second = slot == at_first, slot == at_second
    routing = jnp.sum(
        jnp.where(is_first, share * exp_first, jnp.where(is_second, share * exp_second, 0.0)),
        axis=1,
        keepdims=True,
    )
    pick = jnp.where(is_first | is_second, 1.0, 0.0).astype(BF)
    slots_out[...] = pick
    cols = pl.ds(pl.multiple_of(half * width, width), width)
    packed[:, :width] = dot(pick, rows[:, cols], 1, 0).astype(BF)
    packed[:, width:] = (dot(pick, cots[:, cols], 1, 0) * routing).astype(BF)


def own_kernel(place, own, weights, pre):
    width = own.shape[1] // 2
    cols = pl.ds(pl.multiple_of(place[0] * width, width), width)
    pre[0] = dot(own[:, :width], weights[0, :, cols], 1, 1)
    pre[1] = dot(own[:, :width], weights[1, :, cols], 1, 1)
    pre[2] = dot(own[:, width:], weights[2, :, cols], 1, 1)


def expert_kernel(place, far, weights, pre, part, grads):
    width = far.shape[1] // 2
    cols = pl.ds(pl.multiple_of((1 - place[0]) * width, width), width)
    gate_pre = pre[0] + dot(far[:, :width], weights[0, :, cols], 1, 1)
    up_pre = pre[1] + dot(far[:, :width], weights[1, :, cols], 1, 1)
    back = pre[2] + dot(far[:, width:], weights[2, :, cols], 1, 1)
    sig = jax.nn.sigmoid(gate_pre)
    silu = gate_pre * sig
    gg = (back * up_pre * sig * (1.0 + gate_pre * (1.0 - sig))).astype(BF)
    gu = (back * silu).astype(BF)
    grads[0] = gg
    grads[1] = gu
    grads[2] = (silu * up_pre).astype(BF)
    block = part.shape[2]
    for j in range(part.shape[0]):
        cols = slice(j * block, (j + 1) * block)
        part[j] = (dot(gg, weights[0, :, cols], 1, 0) + dot(gu, weights[1, :, cols], 1, 0)).astype(BF)


def weight_grad_kernel(place, grads, own, far, keep, send):
    width = own.shape[1] // 2
    rows = keep.shape[1]
    for k in range(3):
        lanes = slice(width, 2 * width) if k == 2 else slice(0, width)
        for right, half in ((own, place[0]), (far, 1 - place[0])):
            cols = pl.ds(pl.multiple_of(half * width, width), width)
            both = dot(grads[k], right[:, lanes], 0, 0)
            keep[k, :, cols] = both[:rows]
            send[k, :, cols] = both[rows:].astype(BF)


def call(kernel, outs, *args, near=True):
    vmem = pl.BlockSpec(memory_space=pltpu.VMEM)
    space = pltpu.VMEM if near else pltpu.HBM
    args = args[:1] + tuple(pltpu.with_memory_space_constraint(a, space) for a in args[1:])
    return pl.pallas_call(
        kernel,
        out_shape=tuple((pltpu.VMEM if v else pltpu.HBM)(s, d) for s, d, v in outs),
        in_specs=[pl.BlockSpec(memory_space=pltpu.SMEM)] + [vmem] * (len(args) - 1),
        out_specs=tuple(vmem for _ in outs),
        compiler_params=pltpu.CompilerParams(vmem_limit_bytes=24 << 20),
    )(*args)


def per_device(
    cotangent,
    layer_input,
    group_choice,
    inner_pair,
    group_weight,
    inner_logits,
    w_gate,
    w_up,
    w_down,
    outer_gate,
    inner_gate,
    value_stream,
    conv_out,
    conv_taps,
    w_out,
):
    sp, tp = lax.axis_size("sp"), lax.axis_size("tp")
    at = lax.axis_index("tp")
    chip, core = at // 2, at % 2
    tok, width = cotangent.shape
    hidden = w_gate.shape[1]
    half_width = width // 2
    slots = sp * 8
    col = width // tp
    place = jnp.stack([chip % 2, core]).astype(jnp.int32)
    swap = [(i, i ^ 1) for i in range(tp)]
    onward = [(i, (i + 2 - 4 * (i % 2)) % tp) for i in range(tp)]
    lines = [list(range(c, tp, 2)) for c in range(2)]

    packed, pick = call(
        pack_kernel,
        [((slots, width), BF, False), ((slots, tok), BF, False)],
        place,
        group_choice[None, :],
        inner_pair.T,
        group_weight[None, :],
        inner_logits.T,
        layer_input,
        cotangent,
        near=False,
    )
    own = lax.all_to_all(packed.reshape(sp, 8, width), "sp", 0, 0, tiled=True).reshape(slots, width)
    mine = jnp.concatenate([w_gate, w_up, w_down], axis=0)
    weights = jnp.concatenate([mine, lax.ppermute(mine, "tp", swap)], axis=1)
    far = lax.ppermute(own, "tp", onward)
    (pre,) = call(own_kernel, [((3, slots, 2 * hidden), F32, True)], place, own, weights)
    part, grads = call(
        expert_kernel,
        [((tp // 2, slots, 2 * col), BF, False), ((3, slots, 2 * hidden), BF, True)],
        place,
        far,
        weights,
        pre,
    )
    parts = lax.all_to_all(part, "tp", 0, 0, axis_index_groups=lines, tiled=True)
    keep, send = call(
        weight_grad_kernel,
        [((3, hidden, width), F32, False), ((3, hidden, width), BF, False)],
        place,
        grads,
        own,
        far,
    )
    theirs = lax.ppermute(send, "tp", swap)
    outer_t, conv_t, inner_t, value_t = outer_gate.T, conv_out.T, inner_gate.T, value_stream.T
    mixer_out = (outer_t.astype(F32) * conv_t.astype(F32)).astype(BF)
    outer_t, conv_t, inner_t, value_t, mixer_out, parts = lax.optimization_barrier(
        (outer_t, conv_t, inner_t, value_t, mixer_out, parts)
    )
    shares = jnp.sum(parts.astype(F32), axis=0).astype(BF)
    returned = lax.all_to_all(shares.reshape(sp, 8, 2 * col), "sp", 0, 0, tiled=True)
    back = dot(pick, returned.reshape(slots, 2 * col), 0, 0)
    back_mine = jnp.where(core == 0, back[:, :col], back[:, col:])
    back_theirs = jnp.where(core == 0, back[:, col:], back[:, :col])
    back_other = lax.ppermute(back_theirs, "tp", swap)
    cot_cols = lax.dynamic_slice_in_dim(cotangent, at * col, col, 1).astype(F32)
    own_cols = (cot_cols + back_mine + back_other).astype(BF)
    grad_rows = lax.all_gather(own_cols, "tp", axis=1, tiled=True)
    grad_rows, theirs = lax.optimization_barrier((grad_rows, theirs))
    grad_w = (keep + theirs.astype(F32)).astype(BF)
    partial_out = dot(grad_rows, mixer_out, 0, 0).astype(BF)
    sums = lax.all_to_all(partial_out.reshape(sp, width // sp, -1), "sp", 0, 0, tiled=True)
    grad_w_out = jnp.sum(sums.astype(F32), axis=0)
    grad_out = dot(grad_rows, w_out, 1, 0)
    grad_outer_gate = (grad_out * conv_t.astype(F32)).astype(BF).T
    grad_conv = grad_out * outer_t.astype(F32)
    following = lax.ppermute(grad_conv[: TAPS - 1], "sp", [(i + 1, i) for i in range(sp - 1)])
    extended = jnp.concatenate([grad_conv, following], axis=0)
    grad_mixed = jnp.zeros_like(grad_conv)
    for offset in range(TAPS):
        start = TAPS - 1 - offset
        grad_mixed = grad_mixed + conv_taps[offset][None, :] * extended[start : start + tok]
    grad_inner_gate = (grad_mixed * value_t.astype(F32)).astype(BF).T
    grad_value_stream = (grad_mixed * inner_t.astype(F32)).astype(BF).T
    return (
        own_cols,
        grad_w[0:1],
        grad_w[1:2],
        grad_w[2:3],
        grad_w_out,
        grad_outer_gate,
        grad_inner_gate,
        grad_value_stream,
    )


def solution(mesh):
    tokens, experts, channels = P("sp", None), P("sp", "tp", None), P("tp", "sp")
    return jax.shard_map(
        per_device,
        mesh=mesh,
        in_specs=(tokens, tokens, P("sp"), tokens, P("sp"), tokens)
        + (experts,) * 3
        + (channels,) * 4
        + (P(None, "tp"), P(None, "tp")),
        out_specs=(P("sp", "tp"),) + (experts,) * 3 + (P("sp", "tp"),) + (channels,) * 3,
        check_vma=False,
    )
```

```python
import jax
import jax.numpy as jnp
from jax import lax
from jax.experimental import pallas as pl
from jax.experimental.pallas import tpu as pltpu
from jax.sharding import PartitionSpec as P

TAPS = 3
INNER = 4
BF = jnp.bfloat16
F32 = jnp.float32


def dot(a, b, ca, cb):
    return lax.dot_general(a, b, (((ca,), (cb,)), ((), ())), preferred_element_type=F32)


def pack_kernel(place, group, pair, weight, logits, rows, cots, packed, slots_out):
    half, core = place[0], place[1]
    tokens, width = rows.shape[0], packed.shape[1] // 2
    slots = packed.shape[0]
    experts = slots // 8
    first = INNER * group[...] + pair[0:1, :]
    second = INNER * group[...] + pair[1:2, :]
    kind = lax.broadcasted_iota(jnp.int32, (experts, tokens), 0)
    named_first = (kind == first).astype(F32)
    named_second = (kind == second).astype(F32)
    before = (
        lax.broadcasted_iota(jnp.int32, (tokens, tokens), 0)
        < lax.broadcasted_iota(jnp.int32, (tokens, tokens), 1)
    ).astype(BF)
    rank = dot((named_first + named_second).astype(BF), before, 1, 0)
    rank_first = jnp.sum(rank * named_first, axis=0, keepdims=True).astype(jnp.int32)
    rank_second = jnp.sum(rank * named_second, axis=0, keepdims=True).astype(jnp.int32)
    every = lax.broadcasted_iota(jnp.int32, (2 * slots, tokens), 0)
    slots_out[...] = jnp.where(
        (every == first * 16 + rank_first) | (every == second * 16 + rank_second), 1.0, 0.0
    ).astype(BF)
    rank_first, rank_second = rank_first - 8 * core, rank_second - 8 * core
    at_first = jnp.where((rank_first >= 0) & (rank_first < 8), first * 8 + rank_first, -1)
    at_second = jnp.where((rank_second >= 0) & (rank_second < 8), second * 8 + rank_second, -1)
    top = jnp.maximum(logits[0:1, :], logits[1:2, :])
    exp_first = jnp.exp(logits[0:1, :] - top)
    exp_second = jnp.exp(logits[1:2, :] - top)
    share = weight[...] / (exp_first + exp_second)
    slot = lax.broadcasted_iota(jnp.int32, (slots, tokens), 0)
    is_first, is_second = slot == at_first, slot == at_second
    routing = jnp.sum(
        jnp.where(is_first, share * exp_first, jnp.where(is_second, share * exp_second, 0.0)),
        axis=1,
        keepdims=True,
    )
    pick = jnp.where(is_first | is_second, 1.0, 0.0).astype(BF)
    cols = pl.ds(pl.multiple_of(half * width, width), width)
    packed[:, :width] = dot(pick, rows[:, cols], 1, 0).astype(BF)
    packed[:, width:] = (dot(pick, cots[:, cols], 1, 0) * routing).astype(BF)


def own_kernel(place, own, weights, pre):
    width = own.shape[1] // 2
    cols = pl.ds(pl.multiple_of(place[0] * width, width), width)
    pre[0] = dot(own[:, :width], weights[0, :, cols], 1, 1)
    pre[1] = dot(own[:, :width], weights[1, :, cols], 1, 1)
    pre[2] = dot(own[:, width:], weights[2, :, cols], 1, 1)


def expert_kernel(place, far, weights, pre, part, grads):
    width = far.shape[1] // 2
    cols = pl.ds(pl.multiple_of((1 - place[0]) * width, width), width)
    gate_pre = pre[0] + dot(far[:, :width], weights[0, :, cols], 1, 1)
    up_pre = pre[1] + dot(far[:, :width], weights[1, :, cols], 1, 1)
    back = pre[2] + dot(far[:, width:], weights[2, :, cols], 1, 1)
    sig = jax.nn.sigmoid(gate_pre)
    silu = gate_pre * sig
    gg = (back * up_pre * sig * (1.0 + gate_pre * (1.0 - sig))).astype(BF)
    gu = (back * silu).astype(BF)
    grads[0] = gg
    grads[1] = gu
    grads[2] = (silu * up_pre).astype(BF)
    block = part.shape[2]
    for j in range(0, part.shape[0], 2):
        cols = slice(j * block, (j + 2) * block)
        two = dot(gg, weights[0, :, cols], 1, 0) + dot(gu, weights[1, :, cols], 1, 0)
        part[j] = two[:, :block].astype(BF)
        part[j + 1] = two[:, block:].astype(BF)


def sum_kernel(place, parts, shares):
    count, slots, col = parts.shape
    for core in range(2):
        total = parts[core].astype(F32)
        for k in range(core + 2, count, 2):
            total = total + parts[k].astype(F32)
        shares[:, core] = total.reshape(slots // 8, 8, col).astype(BF)


def weight_grad_kernel(place, grads, own, far, keep, send):
    width = own.shape[1] // 2
    rows = keep.shape[1]
    for k in range(3):
        lanes = slice(width, 2 * width) if k == 2 else slice(0, width)
        for right, half in ((own, place[0]), (far, 1 - place[0])):
            cols = pl.ds(pl.multiple_of(half * width, width), width)
            both = dot(grads[k], right[:, lanes], 0, 0)
            keep[k, :, cols] = both[:rows]
            send[k, :, cols] = both[rows:].astype(BF)


def call(kernel, outs, *args, near=True):
    vmem = pl.BlockSpec(memory_space=pltpu.VMEM)
    space = pltpu.VMEM if near else pltpu.HBM
    args = args[:1] + tuple(pltpu.with_memory_space_constraint(a, space) for a in args[1:])
    return pl.pallas_call(
        kernel,
        out_shape=tuple((pltpu.VMEM if v else pltpu.HBM)(s, d) for s, d, v in outs),
        in_specs=[pl.BlockSpec(memory_space=pltpu.SMEM)] + [vmem] * (len(args) - 1),
        out_specs=tuple(vmem for _ in outs),
        compiler_params=pltpu.CompilerParams(vmem_limit_bytes=24 << 20),
    )(*args)


def per_device(
    cotangent,
    layer_input,
    group_choice,
    inner_pair,
    group_weight,
    inner_logits,
    w_gate,
    w_up,
    w_down,
    outer_gate,
    inner_gate,
    value_stream,
    conv_out,
    conv_taps,
    w_out,
):
    sp, tp = lax.axis_size("sp"), lax.axis_size("tp")
    at = lax.axis_index("tp")
    chip, core = at // 2, at % 2
    tok, width = cotangent.shape
    hidden = w_gate.shape[1]
    slots = sp * 8
    col = width // tp
    place = jnp.stack([chip % 2, core]).astype(jnp.int32)
    swap = [(i, i ^ 1) for i in range(tp)]
    onward = [(i, (i + 2 - 4 * (i % 2)) % tp) for i in range(tp)]

    packed, pick = call(
        pack_kernel,
        [((slots, width), BF, False), ((2 * slots, tok), BF, False)],
        place,
        group_choice[None, :],
        inner_pair.T,
        group_weight[None, :],
        inner_logits.T,
        layer_input,
        cotangent,
        near=False,
    )
    own = lax.all_to_all(packed.reshape(sp, 8, width), "sp", 0, 0, tiled=True).reshape(slots, width)
    mine = jnp.concatenate([w_gate, w_up, w_down], axis=0)
    weights = jnp.concatenate([mine, lax.ppermute(mine, "tp", swap)], axis=1)
    far = lax.ppermute(own, "tp", onward)
    (pre,) = call(own_kernel, [((3, slots, 2 * hidden), F32, True)], place, own, weights)
    part, grads = call(
        expert_kernel,
        [((tp, slots, col), BF, False), ((3, slots, 2 * hidden), BF, True)],
        place,
        far,
        weights,
        pre,
    )
    parts = lax.all_to_all(part, "tp", 0, 0, tiled=True)
    keep, send = call(
        weight_grad_kernel,
        [((3, hidden, width), F32, False), ((3, hidden, width), BF, False)],
        place,
        grads,
        own,
        far,
    )
    theirs = lax.ppermute(send, "tp", swap)
    outer_t, conv_t, inner_t, value_t = outer_gate.T, conv_out.T, inner_gate.T, value_stream.T
    mixer_out = (outer_t.astype(F32) * conv_t.astype(F32)).astype(BF)
    outer_t, conv_t, inner_t, value_t, mixer_out, parts = lax.optimization_barrier(
        (outer_t, conv_t, inner_t, value_t, mixer_out, parts)
    )
    (shares,) = call(sum_kernel, [((sp, 2, 8, col), BF, False)], place, parts)
    returned = lax.all_to_all(shares.reshape(sp, 16, col), "sp", 0, 0, tiled=True)
    back = dot(pick, returned.reshape(2 * slots, col), 0, 0)
    cot_cols = lax.dynamic_slice_in_dim(cotangent, at * col, col, 1).astype(F32)
    own_cols = (cot_cols + back).astype(BF)
    grad_rows = lax.all_gather(own_cols, "tp", axis=1, tiled=True)
    grad_rows, theirs = lax.optimization_barrier((grad_rows, theirs))
    grad_w = (keep + theirs.astype(F32)).astype(BF)
    partial_out = dot(grad_rows, mixer_out, 0, 0).astype(BF)
    grad_rows, partial_out = lax.optimization_barrier((grad_rows, partial_out))
    sums = lax.all_to_all(partial_out.reshape(sp, width // sp, -1), "sp", 0, 0, tiled=True)
    grad_w_out = jnp.sum(sums.astype(F32), axis=0)
    grad_out = dot(grad_rows, w_out, 1, 0)
    grad_outer_gate = (grad_out * conv_t.astype(F32)).astype(BF).T
    grad_conv = grad_out * outer_t.astype(F32)
    following = lax.ppermute(grad_conv[: TAPS - 1], "sp", [(i + 1, i) for i in range(sp - 1)])
    extended = jnp.concatenate([grad_conv, following], axis=0)
    grad_mixed = jnp.zeros_like(grad_conv)
    for offset in range(TAPS):
        start = TAPS - 1 - offset
        grad_mixed = grad_mixed + conv_taps[offset][None, :] * extended[start : start + tok]
    grad_inner_gate = (grad_mixed * value_t.astype(F32)).astype(BF).T
    grad_value_stream = (grad_mixed * inner_t.astype(F32)).astype(BF).T
    return (
        own_cols,
        grad_w[0:1],
        grad_w[1:2],
        grad_w[2:3],
        grad_w_out,
        grad_outer_gate,
        grad_inner_gate,
        grad_value_stream,
    )


def solution(mesh):
    tokens, experts, channels = P("sp", None), P("sp", "tp", None), P("tp", "sp")
    return jax.shard_map(
        per_device,
        mesh=mesh,
        in_specs=(tokens, tokens, P("sp"), tokens, P("sp"), tokens)
        + (experts,) * 3
        + (channels,) * 4
        + (P(None, "tp"), P(None, "tp")),
        out_specs=(P("sp", "tp"),) + (experts,) * 3 + (P("sp", "tp"),) + (channels,) * 3,
        check_vma=False,
    )
```
